32 devices in a mesh: sp: 4 (over y, x), tp: 8 (over z, core).
Axes of the slice: x: 2, y: 2, z: 4, core: 2. Of those that a mesh axis runs over, the one named last changes fastest.
Arguments:
- residual_in: bfloat16 [1024, 4096], P(('sp', 'tp')), may hold values from -6 to 6
- queries: bfloat16 [1024, 2048], P('sp', 'tp'), may hold values from -6 to 6
- keys: bfloat16 [1024, 2048], P('sp', 'tp'), may hold values from -6 to 6
- values: bfloat16 [1024, 2048], P('sp', 'tp'), may hold values from -6 to 6
- break_offset: bfloat16 [1024, 32], P('sp', 'tp'), may hold values from -14 to 1
- doc_ids: int32 [1024], P('sp'), may hold values from 0 to 2, never falling along the last dimension, each value on 1 to 640 neighbouring positions
- out_weight: bfloat16 [2048, 4096], P('tp'), may hold values from -0.125 to 0.125
- norm_gain: float32 [4096], replicated, may hold values from 0.1 to 1.9
- group_router: bfloat16 [4096, 2], replicated, may hold values from -0.1875 to 0.1875
- expert_router: bfloat16 [4096, 4], replicated, may hold values from -0.1875 to 0.1875
- expert_ids: int32 [1024, 2], P('sp'), may hold values from 0 to 3, as said below
- gate_weight: bfloat16 [4, 4096, 4096], P('sp', None, 'tp'), may hold values from -0.09375 to 0.09375
- up_weight: bfloat16 [4, 4096, 4096], P('sp', None, 'tp'), may hold values from -0.09375 to 0.09375
- down_weight: bfloat16 [4, 4096, 4096], P('sp', 'tp'), may hold values from -0.09375 to 0.09375
Outputs:
- layer_out: bfloat16 [1024, 4096], P(('sp', 'tp'))
The draws below stay inside these ranges and needn't reach their ends.
Inputs may be any that keep to these rules, and one draw needn't show every extreme that they name: `doc_ids`: document numbers never fall along the positions; one document covers exactly 640 positions. `expert_ids`: the two experts of a position differ and lie in one group of 2 consecutive numbers; in each aligned block of 32 positions every expert is named exactly 16 times.
All inputs are finite; a program needn't handle non-finite values.
Results may differ from the reference program's by a relative error of at most 0.013.
Values may be sent and summed in bfloat16 or wider, within the bound.
No kernel may reach another device: no remote copies, remote signals or barrier semaphores. Data moves between devices by JAX's collectives and lax.ppermute only.
A program may use at most 64 MiB of HBM per device.

```python
import math
import jax
import jax.numpy as jnp
import numpy as np
from jax import lax

D = 4096
ATTENTION_HEADS = 32
HEAD_DIM = 64
ATT = 2048
D_EXPERT = 4096
GROUPS = 2
EXPERTS = 4
GROUP_EXPERTS = 2
TOK_DEV = 256
SEQUENCE_TOKENS = 1024
ROWS_DEV = 32
KEY_BLOCK = 256
DOCS = 3
DOC_MOST = 640
N_TP = 8


def draw_break_offset(key, part):
    gathered_keys = jax.random.split(jax.random.fold_in(key, 7), 5)
    lagging_heads = jax.random.uniform(gathered_keys[0], (ATTENTION_HEADS,)) < 0.5
    factor = jnp.exp(jax.random.uniform(gathered_keys[1], (SEQUENCE_TOKENS // TOK_DEV, 1), minval=0.0, maxval=math.log(4.0)))
    factor = jnp.repeat(factor, TOK_DEV, axis=0)
    slow_level = jnp.log(0.1 * factor / SEQUENCE_TOKENS)
    fast_level = jnp.log(factor / 48.0)
    jitter = 0.5 * jax.random.normal(gathered_keys[2], (SEQUENCE_TOKENS, ATTENTION_HEADS))
    logging_level = jnp.where(lagging_heads[None, :], slow_level, fast_level) + jitter
    spike_matched = jax.random.uniform(gathered_keys[3], (SEQUENCE_TOKENS, ATTENTION_HEADS)) < 6.0 / SEQUENCE_TOKENS
    spike_value = jax.random.uniform(gathered_keys[4], (SEQUENCE_TOKENS, ATTENTION_HEADS), minval=-1.0, maxval=0.0)
    document_starts = jnp.where(spike_matched & lagging_heads[None, :], spike_value, logging_level)
    return jnp.clip(document_starts, -14.0, 1.0).astype(jnp.bfloat16)


def draw_expert_ids(key, part):
    routing_key = jax.random.fold_in(key, 13)
    blocks = SEQUENCE_TOKENS // ROWS_DEV
    per_group = ROWS_DEV // GROUPS
    group_size = EXPERTS // GROUPS
    block_keys = jax.random.split(routing_key, blocks)

    def one_block(block_key):
        perm_key, relabel_key, swap_key = jax.random.split(block_key, 3)
        row_rank = jax.random.permutation(perm_key, ROWS_DEV)
        group_index = row_rank // per_group
        inner_rank = row_rank % per_group
        relabel = jax.vmap(lambda sub_key: jax.random.permutation(sub_key, group_size))(jax.random.split(relabel_key, GROUPS))
        first = relabel[group_index, inner_rank % group_size]
        second = relabel[group_index, (inner_rank + 1) % group_size]
        swapped = jax.random.randint(swap_key, (ROWS_DEV,), 0, 2)
        lower_id = jnp.where(swapped == 1, second, first)
        upper_id = jnp.where(swapped == 1, first, second)
        return jnp.stack([group_index * group_size + lower_id, group_index * group_size + upper_id], axis=1)
    return jax.vmap(one_block)(block_keys).reshape(SEQUENCE_TOKENS, 2).astype(jnp.int32)


def block_levels(key, shape, shards, smallest, largest):
    loudness, own = 1.0, jax.random.fold_in(key, 6)
    for axis_at, blocks in shards:
        draws = jnp.exp(jax.random.uniform(jax.random.fold_in(own, axis_at), (blocks,), jnp.float32, smallest / len(shards), largest / len(shards)))
        loudness = loudness * jnp.repeat(draws, shape[axis_at] // blocks).reshape([-1 if axis == axis_at else 1 for axis in range(len(shape))])
    return loudness


def profile(amount, total, bound, skew):
    portions = [(1 << 20) // math.isqrt(grade ** skew) + 1 for grade in range(2, amount + 1)]
    surplus, holding = total - bound - (amount - 1), [1] * (amount - 1)
    while surplus > 0:
        movable = [i for i in range(amount - 1) if holding[i] < bound]
        mass, left = sum([portions[i] for i in movable]), surplus
        for i in movable:
            extra = min(bound - holding[i], max(1, left * portions[i] // mass), surplus)
            holding[i] = holding[i] + extra
            surplus = surplus - extra
    return np.array([bound] + holding)


def ragged(rng, amount, total, bound, lean):
    if amount == 2:
        one = jax.random.randint(rng, (), max(1, total - bound), min(bound, total - 1) + 1)
        return jnp.stack([one, total - one])
    lengths = jnp.asarray(profile(amount, total, bound, lean), jnp.int32)
    twos = (amount - 1) // 2
    donor, sink = lengths[1:1 + 2 * twos:2], lengths[2:2 + 2 * twos:2]
    room = jnp.minimum(donor - 1, bound - sink)
    passed = jax.random.randint(jax.random.fold_in(rng, 1), (twos,), 0, 1 << 20) % (room + 1)
    lengths = lengths.at[1:1 + 2 * twos:2].set(donor - passed).at[2:2 + 2 * twos:2].set(sink + passed)
    return lengths[jax.random.permutation(jax.random.fold_in(rng, 2), amount)]


def gaussian(stream_key, dims, width, bound, cuts=(), held_as=jnp.bfloat16):
    result = jax.random.normal(stream_key, dims, jnp.float32) * width
    if len(cuts) > 0:
        result = block_levels(stream_key, dims, cuts, -0.22, 0.18) * result
    return jnp.clip(result, min=-bound, max=bound).astype(held_as)


def setup_inputs(seed: int = 0) -> dict:
    seeds = jax.random.split(jax.random.key(seed), 15)
    return {
        "residual_in": gaussian(seeds[0], (SEQUENCE_TOKENS, D), 1.0, 6.0, ((0, 32),)),
        "queries": gaussian(seeds[1], (SEQUENCE_TOKENS, ATT), 1.0, 6.0, ((0, 4), (1, 8))),
        "keys": gaussian(seeds[2], (SEQUENCE_TOKENS, ATT), 1.0, 6.0, ((0, 4), (1, 8))),
        "values": gaussian(seeds[3], (SEQUENCE_TOKENS, ATT), 1.0, 6.0, ((0, 4), (1, 8))),
        "break_offset": draw_break_offset(jax.random.fold_in(seeds[14], 71), 0),
        "doc_ids": jnp.searchsorted(jnp.cumsum(ragged(seeds[5], DOCS, SEQUENCE_TOKENS, DOC_MOST, 0)), jnp.arange(SEQUENCE_TOKENS), side="right").astype(jnp.int32),
        "out_weight": gaussian(seeds[6], (ATT, D), ATT ** -0.5, 0.125, ((0, 8),)),
        "norm_gain": jnp.clip(1.0 + 0.18 * jax.random.normal(seeds[7], (D,), jnp.float32), 0.1, 1.9),
        "group_router": gaussian(seeds[8], (D, GROUPS), (D // 4) ** -0.5, 0.1875),
        "expert_router": gaussian(seeds[9], (D, EXPERTS), (D // 4) ** -0.5, 0.1875),
        "expert_ids": draw_expert_ids(jax.random.fold_in(seeds[14], 71), 0),
        "gate_weight": gaussian(seeds[11], (EXPERTS, D, D_EXPERT), D ** -0.5, 0.09375, ((0, 4), (2, 8))),
        "up_weight": gaussian(seeds[12], (EXPERTS, D, D_EXPERT), D ** -0.5, 0.09375, ((0, 4), (2, 8))),
        "down_weight": gaussian(seeds[13], (EXPERTS, D_EXPERT, D), D_EXPERT ** -0.5, 0.09375, ((0, 4), (1, 8))),
    }


def block_result(query_head, key_block, value_block, offset_block, query_pos, query_doc, key_pos, key_doc):
    scores = jnp.dot(query_head, key_block.T, preferred_element_type=jnp.float32) * HEAD_DIM ** (-0.5)
    scores = scores + offset_block.astype(jnp.float32)[None, :]
    live_mask = (key_pos[None, :] < query_pos[:, None]) & (key_doc[None, :] == query_doc[:, None])
    stay_log = jnp.where(live_mask, jax.nn.log_sigmoid(-scores), jnp.float32(0.0))
    within = lax.cumsum(stay_log, axis=1, reverse=True) - stay_log
    weights = jnp.where(live_mask, jnp.exp(jax.nn.log_sigmoid(scores) + within), jnp.float32(0.0)).astype(jnp.bfloat16)
    partial_out = jnp.dot(weights, value_block, preferred_element_type=jnp.float32)
    return (partial_out, lax.optimization_barrier(jnp.sum(stay_log, axis=1)))

def attend(queries, keys, values, break_offset, doc_ids):
    positions = jnp.arange(SEQUENCE_TOKENS, dtype=jnp.int32)
    query_heads = queries.reshape(SEQUENCE_TOKENS, ATTENTION_HEADS, HEAD_DIM).transpose(1, 0, 2)
    key_heads = keys.reshape(SEQUENCE_TOKENS, ATTENTION_HEADS, HEAD_DIM).transpose(1, 0, 2)
    value_heads = values.reshape(SEQUENCE_TOKENS, ATTENTION_HEADS, HEAD_DIM).transpose(1, 0, 2)
    document_starts = break_offset.T
    block_count = SEQUENCE_TOKENS // KEY_BLOCK

    def one_head(operands):
        query_head, key_head, value_head, offset_head = operands

        def advance(running, block_index):
            out_sum, stay_sum = running
            block_begin = (block_index * KEY_BLOCK).astype(jnp.int32)
            key_block = lax.dynamic_slice_in_dim(key_head, block_begin, KEY_BLOCK, 0)
            value_block = lax.dynamic_slice_in_dim(value_head, block_begin, KEY_BLOCK, 0)
            offset_block = lax.dynamic_slice_in_dim(offset_head, block_begin, KEY_BLOCK, 0)
            key_doc = lax.dynamic_slice_in_dim(doc_ids, block_begin, KEY_BLOCK, 0)
            key_pos = block_begin + jnp.arange(KEY_BLOCK, dtype=jnp.int32)
            partial_out, totals = block_result(query_head, key_block, value_block, offset_block, positions, doc_ids, key_pos, key_doc)
            out_sum = out_sum + jnp.exp(stay_sum)[:, None] * partial_out
            return ((out_sum, stay_sum + totals), None)
        initial = (jnp.zeros((SEQUENCE_TOKENS, HEAD_DIM), jnp.float32), jnp.zeros((SEQUENCE_TOKENS,), jnp.float32))
        final, unused = lax.scan(advance, initial, jnp.arange(block_count, dtype=jnp.int32), reverse=True)
        return final[0]
    mixed = lax.map(one_head, (query_heads, key_heads, value_heads, document_starts))
    return mixed.transpose(1, 0, 2).reshape(SEQUENCE_TOKENS, ATTENTION_HEADS * HEAD_DIM).astype(jnp.bfloat16)

def reference(residual_in, queries, keys, values, break_offset, doc_ids, out_weight, norm_gain, group_router, expert_router, expert_ids, gate_weight, up_weight, down_weight):
    attended = attend(queries, keys, values, break_offset, doc_ids)
    width_part = ATTENTION_HEADS * HEAD_DIM // N_TP

    def add_group(running, group_index):
        block_begin = (group_index * width_part).astype(jnp.int32)
        part_in = lax.dynamic_slice_in_dim(attended, block_begin, width_part, 1)
        part_weight = lax.dynamic_slice_in_dim(out_weight, block_begin, width_part, 0)
        product = lax.optimization_barrier(jnp.dot(part_in, part_weight, preferred_element_type=jnp.float32).astype(jnp.bfloat16))
        return (running + product.astype(jnp.float32), None)
    summed, unused = lax.scan(add_group, residual_in.astype(jnp.float32), jnp.arange(N_TP, dtype=jnp.int32))
    mixed_stream = summed.astype(jnp.bfloat16)
    stream_f = mixed_stream.astype(jnp.float32)
    scaling = lax.rsqrt(lax.optimization_barrier(jnp.mean(stream_f * stream_f, axis=1, keepdims=True)) + 1e-06)
    normed = (stream_f * scaling * norm_gain[None, :]).astype(jnp.bfloat16)
    group_logits = jnp.dot(normed, group_router, preferred_element_type=jnp.float32)
    expert_logits = jnp.dot(normed, expert_router, preferred_element_type=jnp.float32)
    chosen_group = expert_ids[:, 0] // GROUP_EXPERTS
    margin = group_logits[:, 0] - group_logits[:, 1]
    own_margin = jnp.where(chosen_group == 0, margin, -margin)
    picked = jnp.take_along_axis(expert_logits, expert_ids, axis=1)
    routes = jax.nn.sigmoid(own_margin)[:, None] * jax.nn.sigmoid(picked - picked[:, ::-1])
    flat_ids = expert_ids.reshape(-1)
    per_expert = 2 * SEQUENCE_TOKENS // EXPERTS
    slice_units = D_EXPERT // N_TP

    def one_expert(operands):
        expert_index, gate_part, up_part, down_part = operands
        row_index = jnp.nonzero(flat_ids == expert_index, size=per_expert)[0].astype(jnp.int32)
        row_block = normed[row_index // 2]
        gate_val = jnp.dot(row_block, gate_part, preferred_element_type=jnp.float32)
        up_val = jnp.dot(row_block, up_part, preferred_element_type=jnp.float32)
        hidden = (jax.nn.silu(gate_val) * up_val).astype(jnp.bfloat16)

        def add_slice(running, slice_index):
            block_begin = (slice_index * slice_units).astype(jnp.int32)
            part_hidden = lax.dynamic_slice_in_dim(hidden, block_begin, slice_units, 1)
            part_down = lax.dynamic_slice_in_dim(down_part, block_begin, slice_units, 0)
            product = lax.optimization_barrier(jnp.dot(part_hidden, part_down, preferred_element_type=jnp.float32).astype(jnp.bfloat16))
            return (running + product.astype(jnp.float32), None)
        initial = jnp.zeros((per_expert, D), jnp.float32)
        total_out, unused_slices = lax.scan(add_slice, initial, jnp.arange(N_TP, dtype=jnp.int32))
        return (total_out.astype(jnp.bfloat16), row_index)
    outputs, indices = lax.map(one_expert, (jnp.arange(EXPERTS, dtype=jnp.int32), gate_weight, up_weight, down_weight))
    expert_out = jnp.zeros((SEQUENCE_TOKENS * 2, D), jnp.bfloat16).at[indices.reshape(-1)].set(outputs.reshape(-1, D))
    expert_out = expert_out.reshape(SEQUENCE_TOKENS, 2, D)
    mixture = lax.optimization_barrier(jnp.sum(routes[:, :, None] * expert_out.astype(jnp.float32), axis=1))
    return (stream_f + mixture).astype(jnp.bfloat16)
```

```python
import functools

import jax
import jax.numpy as jnp
from jax import lax
from jax.experimental import pallas as pl
from jax.experimental.pallas import tpu as pltpu
from jax.sharding import PartitionSpec as P

HEAD_DIM = 64
GROUPS = 2
META_ROWS = 16


def attention_kernel(*refs, block_count, heads):
    query_ref, doc_ref = refs[0], refs[1]
    key_refs = refs[2 : 2 + block_count]
    value_refs = refs[2 + block_count : 2 + 2 * block_count]
    meta_refs = refs[2 + 2 * block_count : 2 + 3 * block_count]
    out_ref, acc_ref, carry_ref = refs[2 + 3 * block_count :]
    tok = query_ref.shape[0]
    row = lax.broadcasted_iota(jnp.int32, (tok, tok), 0)
    col = lax.broadcasted_iota(jnp.int32, (tok, tok), 1)
    later = (row > col).astype(jnp.bfloat16)
    query_doc = doc_ref[...]

    def visit(distance):
        key_doc = meta_refs[distance][heads : heads + 1, :].astype(jnp.float32)
        live = key_doc == query_doc
        if distance == 0:
            live = live & (col < row)
        for head in range(heads):
            lanes = slice(head * HEAD_DIM, (head + 1) * HEAD_DIM)
            query = query_ref[:, lanes] * jnp.bfloat16(HEAD_DIM**-0.5)
            scores = lax.dot_general(
                query,
                key_refs[distance][:, lanes],
                (((1,), (1,)), ((), ())),
                preferred_element_type=jnp.float32,
            )
            scores = scores + meta_refs[distance][head : head + 1, :].astype(jnp.float32)
            soft = jnp.maximum(scores, 0.0) + jnp.log(1.0 + jnp.exp(-jnp.abs(scores)))
            stay = jnp.where(live, -soft, 0.0)
            stay_hi = stay.astype(jnp.bfloat16)
            stay_lo = (stay - stay_hi.astype(jnp.float32)).astype(jnp.bfloat16)
            within = jnp.dot(stay_hi, later, preferred_element_type=jnp.float32) + jnp.dot(
                stay_lo, later, preferred_element_type=jnp.float32
            )
            exponent = scores - soft + within
            if distance > 0:
                exponent = exponent + carry_ref[:, head : head + 1]
            weights = jnp.where(live, jnp.exp(exponent), 0.0).astype(jnp.bfloat16)
            part = jnp.dot(
                weights, value_refs[distance][:, lanes], preferred_element_type=jnp.float32
            )
            total = within[:, :1] + stay[:, :1]
            if distance == 0:
                acc_ref[:, lanes] = part
                carry_ref[:, head : head + 1] = total
            else:
                acc_ref[:, lanes] = acc_ref[:, lanes] + part
                carry_ref[:, head : head + 1] = carry_ref[:, head : head + 1] + total

    visit(0)
    first_doc = jnp.min(query_doc)
    for distance in range(1, block_count):
        last_doc = jnp.max(meta_refs[distance][heads : heads + 1, :].astype(jnp.float32))
        pl.when(last_doc == first_doc)(functools.partial(visit, distance))
    out_ref[...] = acc_ref[...].astype(jnp.bfloat16)


def attend(queries, keys, values, break_offset, doc_ids, sp_count):
    tok, width = queries.shape
    heads = break_offset.shape[1]
    doc_mark = doc_ids.astype(jnp.float32) + 1.0
    meta = jnp.concatenate(
        [
            break_offset.T,
            doc_mark.astype(jnp.bfloat16)[None],
            jnp.zeros((META_ROWS - heads - 1, tok), jnp.bfloat16),
        ],
        axis=0,
    )
    key_blocks, value_blocks, meta_blocks = [keys], [values], [meta]
    for distance in range(1, sp_count):
        pairs = [(i, i + distance) for i in range(sp_count - distance)]
        key_blocks.append(lax.ppermute(keys, "sp", pairs))
        value_blocks.append(lax.ppermute(values, "sp", pairs))
        meta_blocks.append(lax.ppermute(meta, "sp", pairs))
    vmem = pl.BlockSpec(memory_space=pltpu.VMEM)
    return pl.pallas_call(
        functools.partial(attention_kernel, block_count=sp_count, heads=heads),
        out_shape=jax.ShapeDtypeStruct((tok, width), jnp.bfloat16),
        in_specs=[vmem] * (2 + 3 * sp_count),
        out_specs=vmem,
        scratch_shapes=[
            pltpu.VMEM((tok, width), jnp.float32),
            pltpu.VMEM((tok, 128), jnp.float32),
        ],
        name="stick_attention",
    )(queries, doc_mark[:, None], *key_blocks, *value_blocks, *meta_blocks)


def tp_pairs(tp_count, step):
    chips = tp_count // 2
    return [(i, (i // 2 + step) % chips * 2 + i % 2) for i in range(tp_count)]


def swap_pairs(tp_count):
    return [(i, i ^ 1) for i in range(tp_count)]


def add_rounded(*parts):
    return sum(part.astype(jnp.float32) for part in parts).astype(jnp.bfloat16)


def chip_sum(own_parts, sibling_parts, tp_count):
    received = [lax.ppermute(part, "tp", swap_pairs(tp_count)) for part in sibling_parts]
    return [(own, other) for own, other in zip(own_parts, received)]


def ring_reduce(pairs_by_step, tp_count):
    chips = tp_count // 2
    far = chips // 2
    width = pairs_by_step[0][0].shape[-1]
    half = width // 2
    far_sum = add_rounded(*pairs_by_step[far])
    up = lax.ppermute(far_sum[..., :half], "tp", tp_pairs(tp_count, 1))
    down = lax.ppermute(far_sum[..., half:], "tp", tp_pairs(tp_count, -1))
    up_is_half = True
    for step in range(far - 1, 0, -1):
        up_parts, down_parts = pairs_by_step[step], pairs_by_step[chips - step]
        if up_is_half:
            up_sum = [add_rounded(*[p[..., :half] for p in up_parts], up)]
            up_sum.append(add_rounded(*[p[..., half:] for p in up_parts]))
            down_sum = [add_rounded(*[p[..., :half] for p in down_parts])]
            down_sum.append(add_rounded(*[p[..., half:] for p in down_parts], down))
        else:
            up_sum = [add_rounded(*[p[..., :half] for p in up_parts], up[..., :half])]
            up_sum.append(add_rounded(*[p[..., half:] for p in up_parts], up[..., half:]))
            down_sum = [add_rounded(*[p[..., :half] for p in down_parts], down[..., :half])]
            down_sum.append(add_rounded(*[p[..., half:] for p in down_parts], down[..., half:]))
        up = lax.ppermute(jnp.concatenate(up_sum, axis=-1), "tp", tp_pairs(tp_count, 1))
        down = lax.ppermute(jnp.concatenate(down_sum, axis=-1), "tp", tp_pairs(tp_count, -1))
        up_is_half = False
    if up_is_half:
        joined = jnp.concatenate([up, down], axis=-1)
        return list(pairs_by_step[0]) + [joined]
    return list(pairs_by_step[0]) + [up, down]


def ring_gather(block, tp_count):
    chips = tp_count // 2
    far = chips // 2
    half = block.shape[-1] // 2
    blocks = [None] * chips
    blocks[0] = block
    up, down = block, block
    for step in range(1, far):
        up = lax.ppermute(up, "tp", tp_pairs(tp_count, 1))
        down = lax.ppermute(down, "tp", tp_pairs(tp_count, -1))
        blocks[step] = up
        blocks[chips - step] = down
    far_up = lax.ppermute(up[..., :half], "tp", tp_pairs(tp_count, 1))
    far_down = lax.ppermute(down[..., half:], "tp", tp_pairs(tp_count, -1))
    blocks[far] = jnp.concatenate([far_up, far_down], axis=-1)
    return blocks


def rotate_to(rows, begin, axis=0):
    doubled = jnp.concatenate([rows, rows], axis=axis)
    return lax.dynamic_slice_in_dim(doubled, begin, rows.shape[axis], axis)


def normalize(rows, norm_gain):
    rows_f = rows.astype(jnp.float32)
    scaling = lax.rsqrt(jnp.mean(rows_f * rows_f, axis=1, keepdims=True) + 1e-06)
    return (rows_f * scaling * norm_gain[None, :]).astype(jnp.bfloat16)


def route_weights(normed, group_router, expert_router, chosen, group_size):
    group_logits = jnp.dot(normed, group_router, preferred_element_type=jnp.float32)
    expert_logits = jnp.dot(normed, expert_router, preferred_element_type=jnp.float32)
    chosen_group = chosen[:, 0] // group_size
    margin = group_logits[:, 0] - group_logits[:, 1]
    own_margin = jnp.where(chosen_group == 0, margin, -margin)
    experts_iota = jnp.arange(expert_logits.shape[1], dtype=jnp.int32)
    picked = jnp.sum(
        jnp.where(
            chosen[:, :, None] == experts_iota[None, None, :],
            expert_logits[:, None, :],
            jnp.float32(0.0),
        ),
        axis=2,
    )
    return jax.nn.sigmoid(own_margin)[:, None] * jax.nn.sigmoid(picked - picked[:, ::-1])


def slot_table(chosen, expert_count, slots):
    flat_ids = chosen.reshape(-1)
    onehot = (flat_ids[:, None] == jnp.arange(expert_count, dtype=jnp.int32)[None, :]).astype(
        jnp.int32
    )
    before = jnp.cumsum(onehot, axis=0) - onehot
    ranks = jnp.sum(before * onehot, axis=1)
    return (flat_ids * slots + ranks).reshape(chosen.shape)


def expert_rows(row_block, gate_part, up_part, down_part):
    gate_val = jnp.dot(row_block, gate_part, preferred_element_type=jnp.float32)
    up_val = jnp.dot(row_block, up_part, preferred_element_type=jnp.float32)
    hidden = (jax.nn.silu(gate_val) * up_val).astype(jnp.bfloat16)
    return jnp.dot(hidden, down_part, preferred_element_type=jnp.float32).astype(jnp.bfloat16)


def per_device(
    residual_in,
    queries,
    keys,
    values,
    break_offset,
    doc_ids,
    out_weight,
    norm_gain,
    group_router,
    expert_router,
    expert_ids,
    gate_weight,
    up_weight,
    down_weight,
):
    tok_dev, att_width = queries.shape
    width = residual_in.shape[1]
    sp_count = lax.axis_size("sp")
    tp_count = lax.axis_size("tp")
    sp_rank = lax.axis_index("sp")
    tp_rank = lax.axis_index("tp")
    chips = tp_count // 2
    chip, core = tp_rank // 2, tp_rank % 2
    rows_dev = tok_dev // tp_count
    expert_count = sp_count * gate_weight.shape[0]
    group_size = expert_count // GROUPS
    slots = 2 * rows_dev // expert_count

    chosen = lax.dynamic_slice_in_dim(expert_ids, tp_rank * rows_dev, rows_dev, 0)
    slot_ids = slot_table((chosen - sp_rank) % expert_count, expert_count, slots)
    slot_iota = jnp.arange(expert_count * slots, dtype=jnp.int32)
    in_slot = slot_ids[:, :, None] == slot_iota[None, None, :]

    attended = attend(queries, keys, values, break_offset, doc_ids, sp_count)
    by_chip = rotate_to(attended.reshape(chips, 2, rows_dev, att_width), chip)
    projected = []
    for target in (1 - core, core):
        rows = lax.dynamic_index_in_dim(by_chip, target, 1, keepdims=False)
        product = jnp.dot(
            rows.reshape(-1, att_width), out_weight, preferred_element_type=jnp.float32
        )
        projected.append(product.astype(jnp.bfloat16).reshape(chips, rows_dev, width))
    sibling_parts, own_parts = projected
    addends = ring_reduce(
        chip_sum(
            [own_parts[d] for d in range(chips)],
            [sibling_parts[d] for d in range(chips)],
            tp_count,
        ),
        tp_count,
    )
    summed = sum(part.astype(jnp.float32) for part in addends)
    mixed_stream = (residual_in.astype(jnp.float32) + summed).astype(jnp.bfloat16)
    normed = normalize(mixed_stream, norm_gain)
    sent = jnp.dot(
        jnp.any(in_slot, axis=1).astype(jnp.bfloat16).T,
        normed,
        preferred_element_type=jnp.float32,
    ).astype(jnp.bfloat16)
    sent = sent.reshape(expert_count, slots, width)
    arrived = [sent[0]]
    for d in range(1, sp_count):
        pairs = [(i, (i + d) % sp_count) for i in range(sp_count)]
        arrived.append(lax.ppermute(sent[d], "sp", pairs))
    block = jnp.concatenate(arrived, axis=0)
    block_rows = block.shape[0]
    own_blocks = ring_gather(block, tp_count)
    sibling_blocks = [lax.ppermute(b, "tp", swap_pairs(tp_count)) for b in own_blocks]

    far = chips // 2
    near = [d for d in range(chips) if d != far]
    own_out, sibling_out = [None] * chips, [None] * chips
    for steps in (near, [far]):
        fanned = jnp.concatenate(
            [own_blocks[d] for d in steps] + [sibling_blocks[d] for d in steps], axis=0
        )
        partial_out = expert_rows(fanned, gate_weight[0], up_weight[0], down_weight[0])
        parts = partial_out.reshape(2, len(steps), block_rows, width)
        for at, d in enumerate(steps):
            own_out[d], sibling_out[d] = parts[0, at], parts[1, at]
    back = [(chips - d) % chips for d in range(chips)]
    addends = ring_reduce(
        chip_sum([own_out[d] for d in back], [sibling_out[d] for d in back], tp_count), tp_count
    )
    unit_total = add_rounded(*addends).reshape(sp_count, slots, width)
    returned = [unit_total[0]]
    for d in range(1, sp_count):
        pairs = [(i, (i - d) % sp_count) for i in range(sp_count)]
        returned.append(lax.ppermute(unit_total[d], "sp", pairs))
    returned = jnp.concatenate(returned, axis=0)

    routes = route_weights(normed, group_router, expert_router, chosen, group_size)
    placed = jnp.sum(jnp.where(in_slot, routes[:, :, None], jnp.float32(0.0)), axis=1)
    placed_hi = lax.reduce_precision(placed, 8, 7)
    split = jnp.concatenate([placed_hi, placed - placed_hi], axis=0).astype(jnp.bfloat16)
    mixture = jnp.dot(split, returned, preferred_element_type=jnp.float32)
    mixture = mixture[:rows_dev] + mixture[rows_dev:]
    return (mixed_stream.astype(jnp.float32) + mixture).astype(jnp.bfloat16)


def solution(mesh):
    return jax.shard_map(
        per_device,
        mesh=mesh,
        in_specs=(
            P(("sp", "tp"), None),
            P("sp", "tp"),
            P("sp", "tp"),
            P("sp", "tp"),
            P("sp", "tp"),
            P("sp"),
            P("tp", None),
            P(),
            P(),
            P(),
            P("sp", None),
            P("sp", None, "tp"),
            P("sp", None, "tp"),
            P("sp", "tp", None),
        ),
        out_specs=P(("sp", "tp"), None),
        check_vma=False,
    )
```

```python
import functools

import jax
import jax.numpy as jnp
from jax import lax
from jax.experimental import pallas as pl
from jax.experimental.pallas import tpu as pltpu
from jax.sharding import PartitionSpec as P

HEAD_DIM = 64
GROUPS = 2
META_ROWS = 16


def block_visit(distance, query_ref, query_doc, packed_ref, acc_ref, carry_ref, heads):
    tok, width = query_ref.shape
    pieces = tok // width if tok > width else 1
    piece = tok // pieces
    row = lax.broadcasted_iota(jnp.int32, (tok, tok), 0)
    col = lax.broadcasted_iota(jnp.int32, (tok, tok), 1)
    later = (row > col).astype(jnp.bfloat16)

    def meta_row(index):
        found = []
        for at in range(pieces):
            line = 2 * tok + at * META_ROWS + index
            found.append(packed_ref[line : line + 1, :piece].astype(jnp.float32))
        return found[0] if pieces == 1 else jnp.concatenate(found, axis=1)

    live = meta_row(heads) == query_doc
    if distance == 0:
        live = live & (col < row)
    for head in range(heads):
        lanes = slice(head * HEAD_DIM, (head + 1) * HEAD_DIM)
        query = query_ref[:, lanes] * jnp.bfloat16(HEAD_DIM**-0.5)
        scores = lax.dot_general(
            query,
            packed_ref[:tok, lanes],
            (((1,), (1,)), ((), ())),
            preferred_element_type=jnp.float32,
        )
        scores = scores + meta_row(head)
        soft = jnp.maximum(scores, 0.0) + jnp.log(1.0 + jnp.exp(-jnp.abs(scores)))
        stay = jnp.where(live, -soft, 0.0)
        stay_hi = stay.astype(jnp.bfloat16)
        stay_lo = (stay - stay_hi.astype(jnp.float32)).astype(jnp.bfloat16)
        within = jnp.dot(stay_hi, later, preferred_element_type=jnp.float32) + jnp.dot(
            stay_lo, later, preferred_element_type=jnp.float32
        )
        exponent = scores - soft + within
        if distance > 0:
            exponent = exponent + carry_ref[:, head : head + 1]
        weights = jnp.where(live, jnp.exp(exponent), 0.0).astype(jnp.bfloat16)
        part = jnp.dot(
            weights, packed_ref[tok : 2 * tok, lanes], preferred_element_type=jnp.float32
        )
        total = within[:, :1] + stay[:, :1]
        if distance == 0:
            acc_ref[:, lanes] = part
            carry_ref[:, head : head + 1] = total
        else:
            acc_ref[:, lanes] = acc_ref[:, lanes] + part
            carry_ref[:, head : head + 1] = carry_ref[:, head : head + 1] + total


def own_kernel(query_ref, doc_ref, packed_ref, acc_ref, carry_ref, *, heads):
    carry_ref[...] = jnp.zeros(carry_ref.shape, jnp.float32)
    block_visit(0, query_ref, doc_ref[...], packed_ref, acc_ref, carry_ref, heads)


def earlier_kernel(query_ref, doc_ref, acc_in, carry_in, *refs, heads):
    packed_refs, (out_ref, acc_ref, carry_ref) = refs[:-3], refs[-3:]
    acc_ref[...] = acc_in[...]
    carry_ref[...] = carry_in[...]
    query_doc = doc_ref[...]
    first_doc = jnp.min(query_doc)
    tok = query_ref.shape[0]
    for at, packed_ref in enumerate(packed_refs):
        marks = [
            packed_ref[line : line + 1, :].astype(jnp.float32)
            for line in range(2 * tok + heads, packed_ref.shape[0], META_ROWS)
        ]
        last_doc = jnp.max(functools.reduce(jnp.maximum, marks))
        visit = functools.partial(
            block_visit, at + 1, query_ref, query_doc, packed_ref, acc_ref, carry_ref, heads
        )
        pl.when(last_doc == first_doc)(visit)
    out_ref[...] = acc_ref[...].astype(jnp.bfloat16)


def attend(queries, keys, values, break_offset, doc_ids, sp_count):
    tok, width = queries.shape
    heads = break_offset.shape[1]
    doc_mark = doc_ids.astype(jnp.float32) + 1.0
    meta = jnp.concatenate(
        [
            break_offset.T,
            doc_mark.astype(jnp.bfloat16)[None],
            jnp.zeros((META_ROWS - heads - 1, tok), jnp.bfloat16),
        ],
        axis=0,
    )
    if tok > width:
        meta = jnp.concatenate(
            [meta[:, at : at + width] for at in range(0, tok, width)], axis=0
        )
    elif tok < width:
        meta = jnp.pad(meta, ((0, 0), (0, width - tok)))
    packed = jnp.concatenate([keys, values, meta], axis=0)
    received = []
    for distance in range(1, sp_count):
        pairs = [(i, i + distance) for i in range(sp_count - distance)]
        received.append(lax.ppermute(packed, "sp", pairs))
    vmem = pl.BlockSpec(memory_space=pltpu.VMEM)
    state = [
        jax.ShapeDtypeStruct((tok, width), jnp.float32),
        jax.ShapeDtypeStruct((tok, 128), jnp.float32),
    ]
    cost = pl.CostEstimate(
        flops=heads * tok * tok * 700, bytes_accessed=tok * width * 8, transcendentals=0
    )
    acc, carry = pl.pallas_call(
        functools.partial(own_kernel, heads=heads),
        out_shape=state,
        in_specs=[vmem] * 3,
        out_specs=[vmem] * 2,
        cost_estimate=cost,
        name="own_attention",
    )(queries, doc_mark[:, None], packed)
    return pl.pallas_call(
        functools.partial(earlier_kernel, heads=heads),
        out_shape=jax.ShapeDtypeStruct((tok, width), jnp.bfloat16),
        in_specs=[vmem] * (4 + len(received)),
        out_specs=vmem,
        scratch_shapes=[
            pltpu.VMEM((tok, width), jnp.float32),
            pltpu.VMEM((tok, 128), jnp.float32),
        ],
        cost_estimate=cost,
        name="earlier_attention",
    )(queries, doc_mark[:, None], acc, carry, *received)


def tp_pairs(tp_count, step):
    chips = tp_count // 2
    return [(i, (i // 2 + step) % chips * 2 + i % 2) for i in range(tp_count)]


def swap_pairs(tp_count):
    return [(i, i ^ 1) for i in range(tp_count)]


def add_rounded(*parts):
    return sum(part.astype(jnp.float32) for part in parts).astype(jnp.bfloat16)


def chip_sum(own_parts, sibling_parts, tp_count):
    received = [lax.ppermute(part, "tp", swap_pairs(tp_count)) for part in sibling_parts]
    return [(own, other) for own, other in zip(own_parts, received)]


def ring_reduce(pairs_by_step, tp_count):
    chips = tp_count // 2
    far = chips // 2
    width = pairs_by_step[0][0].shape[-1]
    half = width // 2
    far_sum = add_rounded(*pairs_by_step[far])
    up = lax.ppermute(far_sum[..., :half], "tp", tp_pairs(tp_count, 1))
    down = lax.ppermute(far_sum[..., half:], "tp", tp_pairs(tp_count, -1))
    up_is_half = True
    for step in range(far - 1, 0, -1):
        up_parts, down_parts = pairs_by_step[step], pairs_by_step[chips - step]
        if up_is_half:
            up_sum = [add_rounded(*[p[..., :half] for p in up_parts], up)]
            up_sum.append(add_rounded(*[p[..., half:] for p in up_parts]))
            down_sum = [add_rounded(*[p[..., :half] for p in down_parts])]
            down_sum.append(add_rounded(*[p[..., half:] for p in down_parts], down))
        else:
            up_sum = [add_rounded(*[p[..., :half] for p in up_parts], up[..., :half])]
            up_sum.append(add_rounded(*[p[..., half:] for p in up_parts], up[..., half:]))
            down_sum = [add_rounded(*[p[..., :half] for p in down_parts], down[..., :half])]
            down_sum.append(add_rounded(*[p[..., half:] for p in down_parts], down[..., half:]))
        up = lax.ppermute(jnp.concatenate(up_sum, axis=-1), "tp", tp_pairs(tp_count, 1))
        down = lax.ppermute(jnp.concatenate(down_sum, axis=-1), "tp", tp_pairs(tp_count, -1))
        up_is_half = False
    if up_is_half:
        joined = jnp.concatenate([up, down], axis=-1)
        return list(pairs_by_step[0]) + [joined]
    return list(pairs_by_step[0]) + [up, down]


def ring_gather(block, tp_count):
    chips = tp_count // 2
    far = chips // 2
    half = block.shape[-1] // 2
    blocks = [None] * chips
    blocks[0] = block
    up, down = block, block
    for step in range(1, far):
        up = lax.ppermute(up, "tp", tp_pairs(tp_count, 1))
        down = lax.ppermute(down, "tp", tp_pairs(tp_count, -1))
        blocks[step] = up
        blocks[chips - step] = down
    far_up = lax.ppermute(up[..., :half], "tp", tp_pairs(tp_count, 1))
    far_down = lax.ppermute(down[..., half:], "tp", tp_pairs(tp_count, -1))
    blocks[far] = jnp.concatenate([far_up, far_down], axis=-1)
    return blocks


def rotate_to(rows, begin, axis=0):
    doubled = jnp.concatenate([rows, rows], axis=axis)
    return lax.dynamic_slice_in_dim(doubled, begin, rows.shape[axis], axis)


def normalize(rows, norm_gain):
    rows_f = rows.astype(jnp.float32)
    scaling = lax.rsqrt(jnp.mean(rows_f * rows_f, axis=1, keepdims=True) + 1e-06)
    return (rows_f * scaling * norm_gain[None, :]).astype(jnp.bfloat16)


def route_weights(normed, group_router, expert_router, chosen, group_size):
    group_logits = jnp.dot(normed, group_router, preferred_element_type=jnp.float32)
    expert_logits = jnp.dot(normed, expert_router, preferred_element_type=jnp.float32)
    chosen_group = chosen[:, 0] // group_size
    margin = group_logits[:, 0] - group_logits[:, 1]
    own_margin = jnp.where(chosen_group == 0, margin, -margin)
    experts_iota = jnp.arange(expert_logits.shape[1], dtype=jnp.int32)
    picked = jnp.sum(
        jnp.where(
            chosen[:, :, None] == experts_iota[None, None, :],
            expert_logits[:, None, :],
            jnp.float32(0.0),
        ),
        axis=2,
    )
    return jax.nn.sigmoid(own_margin)[:, None] * jax.nn.sigmoid(picked - picked[:, ::-1])


def slot_table(chosen, expert_count, slots):
    flat_ids = chosen.reshape(-1)
    onehot = (flat_ids[:, None] == jnp.arange(expert_count, dtype=jnp.int32)[None, :]).astype(
        jnp.int32
    )
    before = jnp.cumsum(onehot, axis=0) - onehot
    ranks = jnp.sum(before * onehot, axis=1)
    return (flat_ids * slots + ranks).reshape(chosen.shape)


def expert_hidden(row_block, gate_part, up_part):
    gate_val = jnp.dot(row_block, gate_part, preferred_element_type=jnp.float32)
    up_val = jnp.dot(row_block, up_part, preferred_element_type=jnp.float32)
    return (jax.nn.silu(gate_val) * up_val).astype(jnp.bfloat16)


def per_device(
    residual_in,
    queries,
    keys,
    values,
    break_offset,
    doc_ids,
    out_weight,
    norm_gain,
    group_router,
    expert_router,
    expert_ids,
    gate_weight,
    up_weight,
    down_weight,
):
    tok_dev, att_width = queries.shape
    width = residual_in.shape[1]
    sp_count = lax.axis_size("sp")
    tp_count = lax.axis_size("tp")
    sp_rank = lax.axis_index("sp")
    tp_rank = lax.axis_index("tp")
    chips = tp_count // 2
    chip, core = tp_rank // 2, tp_rank % 2
    rows_dev = tok_dev // tp_count
    expert_count = sp_count * gate_weight.shape[0]
    group_size = expert_count // GROUPS
    slots = 2 * rows_dev // expert_count

    chosen = lax.dynamic_slice_in_dim(expert_ids, tp_rank * rows_dev, rows_dev, 0)
    slot_ids = slot_table((chosen - sp_rank) % expert_count, expert_count, slots)
    slot_iota = jnp.arange(expert_count * slots, dtype=jnp.int32)
    in_slot = slot_ids[:, :, None] == slot_iota[None, None, :]

    attended = attend(queries, keys, values, break_offset, doc_ids, sp_count)
    by_chip = rotate_to(attended.reshape(chips, 2, rows_dev, att_width), chip)
    projected = []
    for target in (1 - core, core):
        rows = lax.dynamic_index_in_dim(by_chip, target, 1, keepdims=False)
        product = jnp.dot(
            rows.reshape(-1, att_width), out_weight, preferred_element_type=jnp.float32
        )
        projected.append(product.astype(jnp.bfloat16).reshape(chips, rows_dev, width))
    sibling_parts, own_parts = projected
    addends = ring_reduce(
        chip_sum(
            [own_parts[d] for d in range(chips)],
            [sibling_parts[d] for d in range(chips)],
            tp_count,
        ),
        tp_count,
    )
    summed = sum(part.astype(jnp.float32) for part in addends)
    mixed_stream = (residual_in.astype(jnp.float32) + summed).astype(jnp.bfloat16)
    normed = normalize(mixed_stream, norm_gain)
    sent = jnp.dot(
        jnp.any(in_slot, axis=1).astype(jnp.bfloat16).T,
        normed,
        preferred_element_type=jnp.float32,
    ).astype(jnp.bfloat16)
    sent = sent.reshape(expert_count, slots, width)
    arrived = [sent[0]]
    for d in range(1, sp_count):
        pairs = [(i, (i + d) % sp_count) for i in range(sp_count)]
        arrived.append(lax.ppermute(sent[d], "sp", pairs))
    block = jnp.concatenate(arrived, axis=0)
    block_rows = block.shape[0]
    own_blocks = ring_gather(block, tp_count)
    sibling_blocks = [lax.ppermute(b, "tp", swap_pairs(tp_count)) for b in own_blocks]

    far = chips // 2
    order = [far] + [d for d in range(chips) if d != far]
    fanned = jnp.concatenate(
        [sibling_blocks[d] for d in order] + [own_blocks[d] for d in order], axis=0
    )
    hidden = expert_hidden(fanned, gate_weight[0], up_weight[0])
    outs = []
    for half in (hidden[: chips * block_rows], hidden[chips * block_rows :]):
        part = jnp.dot(half, down_weight[0], preferred_element_type=jnp.float32)
        part = part.astype(jnp.bfloat16).reshape(chips, block_rows, width)
        outs.append([part[order.index((chips - d) % chips)] for d in range(chips)])
    addends = ring_reduce(chip_sum(outs[1], outs[0], tp_count), tp_count)
    unit_total = add_rounded(*addends).reshape(sp_count, slots, width)
    returned = [unit_total[0]]
    for d in range(1, sp_count):
        pairs = [(i, (i - d) % sp_count) for i in range(sp_count)]
        returned.append(lax.ppermute(unit_total[d], "sp", pairs))
    returned = jnp.concatenate(returned, axis=0)

    routes = route_weights(normed, group_router, expert_router, chosen, group_size)
    placed = jnp.sum(jnp.where(in_slot, routes[:, :, None], jnp.float32(0.0)), axis=1)
    placed_hi = lax.reduce_precision(placed, 8, 7)
    split = jnp.concatenate([placed_hi, placed - placed_hi], axis=0).astype(jnp.bfloat16)
    mixture = jnp.dot(split, returned, preferred_element_type=jnp.float32)
    mixture = mixture[:rows_dev] + mixture[rows_dev:]
    return (mixed_stream.astype(jnp.float32) + mixture).astype(jnp.bfloat16)


def solution(mesh):
    return jax.shard_map(
        per_device,
        mesh=mesh,
        in_specs=(
            P(("sp", "tp"), None),
            P("sp", "tp"),
            P("sp", "tp"),
            P("sp", "tp"),
            P("sp", "tp"),
            P("sp"),
            P("tp", None),
            P(),
            P(),
            P(),
            P("sp", None),
            P("sp", None, "tp"),
            P("sp", None, "tp"),
            P("sp", "tp", None),
        ),
        out_specs=P(("sp", "tp"), None),
        check_vma=False,
    )
```
